32 devices in a mesh: ep: 8 (over z, x), tp: 4 (over y, core).
Axes of the slice: x: 2, y: 2, z: 4, core: 2. Of those that a mesh axis runs over, the one named last changes fastest.
Arguments:
- x_mix: bfloat16 [2048, 2048], P('ep'), may hold values from -6 to 6
- mix_gain: float32 [2048], replicated, may hold values from 0.1 to 1.9
- w_query: bfloat16 [2048, 2048], P(None, 'tp'), may hold values from -0.125 to 0.125
- w_key: bfloat16 [2048, 2048], P(None, 'tp'), may hold values from -0.125 to 0.125
- w_value: bfloat16 [2048, 2048], P(None, 'tp'), may hold values from -0.125 to 0.125
- query_gain: float32 [64], replicated, may hold values from 1 to 1.8
- key_gain: float32 [64], replicated, may hold values from 1 to 1.8
- mix_lambda: float32 [16], P('tp'), may hold values from 0.3 to 0.8
- head_gain: float32 [128], replicated, may hold values from 0.1 to 1.9
- w_mix_out: bfloat16 [2048, 2048], P(None, 'tp'), may hold values from -0.125 to 0.125
- x_exp: bfloat16 [1024, 2048], P('ep'), may hold values from -6 to 6
- exp_gain: float32 [2048], replicated, may hold values from 0.1 to 1.9
- routes: int32 [1024, 4], P('ep'), may hold values from 0 to 7, all different within a row; in each aligned block of 128 rows (0 to 127, 128 to 255, ...) at most 96 rows name the same one
- route_weight: float32 [1024, 4], P('ep'), may hold values from 0.1 to 1
- w_gate: bfloat16 [8, 2048, 2048], P('ep', None, 'tp'), may hold values from -0.375 to 0.375
- w_up: bfloat16 [8, 2048, 2048], P('ep', None, 'tp'), may hold values from -0.375 to 0.375
- w_down: bfloat16 [8, 2048, 2048], P('ep', None, 'tp'), may hold values from -0.03125 to 0.03125
Outputs:
- attn_out: bfloat16 [2048, 2048], P('ep', 'tp')
- moe_out: bfloat16 [1024, 2048], P('ep', 'tp')
The draws below stay inside these ranges and needn't reach their ends.
Inputs may be any that keep to these rules, and one draw needn't show every extreme that they name: `routes`: each row names 4 different experts. In each aligned block of 128 rows (the rows of one index of ep), no expert is named by more than 96 rows, a bound that some block reaches.
All inputs are finite; a program needn't handle non-finite values.
Results may differ from the reference program's by a relative error of at most 0.011.
Values may be sent and summed in bfloat16 or wider, within the bound.
A program may use at most 128 MiB of HBM per device.

```python
import math
from functools import partial
import jax
import jax.numpy as jnp
import numpy as np
from jax import lax

D = 2048
HEADS = 16
HEAD = 64
FF = 2048
TOPK = 4
TOK_B = 128
TOKENS_A = 2048
TOKENS_B = 1024
EXPERTS = 8
CAP = 96
N_EP = 8


def levels(own_key, shape, pieces, low, high):
    loudness = 1.0
    for dim, parts in pieces:
        steps = jax.random.uniform(jax.random.fold_in(jax.random.fold_in(own_key, 6), dim), (parts,), jnp.float32, low / len(pieces), high / len(pieces))
        loudness = loudness * jnp.repeat(jnp.exp(steps), shape[dim] // parts).reshape((-1,) + (1,) * (len(shape) - 1 - dim))
    return loudness


def assign_block(key, own, number, rows, amount, top, limit, slope):
    ranking = jax.random.permutation(key, amount)
    crowded, ordinary = load_shares(amount, rows * top, limit, slope, True), load_shares(amount, rows * top, limit, slope, False)
    places = jnp.arange(amount)

    def named(tallies, turn):
        used = int((tallies > 0).sum())
        fixed = max(1, used // 4)
        moved = fixed + (places - fixed + turn * (used - fixed)) % max(1, amount - fixed)
        return jnp.zeros((amount,), jnp.int32).at[ranking[jnp.where(places < fixed, places, moved)]].set(jnp.asarray(tallies, jnp.int32))

    tallies = jnp.where(number % 4 == 0, named(crowded, number // 4), named(ordinary, number - number // 4 - 1))
    mixed = jax.random.permutation(jax.random.fold_in(own, 3), amount)
    donor, receiver = mixed[0:amount // 2 * 2:2], mixed[1:amount // 2 * 2:2]
    slack = jnp.minimum(tallies[donor] - 1, limit - tallies[receiver]) // 2
    slack = jnp.where((donor == ranking[0]) | (receiver == ranking[0]) | (tallies[receiver] == 0), 0, jnp.maximum(slack, 0))
    moved = jax.random.randint(jax.random.fold_in(own, 4), (amount // 2,), 0, 1 << 20) % (slack + 1)
    tallies = tallies.at[donor].add(-moved).at[receiver].add(moved)
    labels = jnp.searchsorted(jnp.cumsum(tallies), jnp.arange(rows * top), side="right").astype(jnp.int32)
    listing = labels.reshape(top, rows).T
    listing = listing[jax.random.permutation(jax.random.fold_in(own, 1), rows)]
    turn = jax.random.randint(jax.random.fold_in(own, 2), (rows, 1), 0, top)
    return jnp.take_along_axis(listing, (jnp.arange(top)[None, :] + turn) % top, axis=1)


def load_shares(amount, total, most, lean, full):
    portions = [(1 << 20) // math.isqrt(grade ** lean) + 1 for grade in range(1, amount + 1)]
    largest = most if full else min(most, max(-(-total // amount), total * portions[0] // sum(portions)))
    least = 1 if total - largest >= amount - 1 else 0
    counts, spare = [largest] + [least] * (amount - 1), total - largest - least * (amount - 1)
    while spare > 0:
        candidates = [i for i in range(1, amount) if counts[i] < largest] or [i for i in range(1, amount) if counts[i] < most]
        pool, budget = sum([portions[i] for i in candidates]), spare
        for i in candidates:
            addition = min(most - counts[i], max(1, budget * portions[i] // pool), spare)
            counts[i] = counts[i] + addition
            spare = spare - addition
    return np.array(counts)


def scatter_about(own_key, dims, spread, most, shards=(), kind=jnp.bfloat16):
    values = spread * jax.random.normal(own_key, dims, jnp.float32)
    if shards:
        values = values * levels(own_key, dims, shards, -0.22, 0.18)
    return jnp.clip(values, -most, most).astype(kind)


def setup_inputs(seed: int = 0) -> dict:
    key_of = jax.random.split(jax.random.key(seed), 18)
    x_mix = scatter_about(key_of[0], (TOKENS_A, D), 1.0, 6.0, ((0, 8),))
    mix_gain = jnp.clip(1.0 + 0.18 * jax.random.normal(key_of[1], (D,), jnp.float32), 0.1, 1.9)
    w_query = scatter_about(key_of[2], (D, HEADS * 2 * HEAD), D ** -0.5, 0.125, ((1, 4),))
    w_key = scatter_about(key_of[3], (D, HEADS * 2 * HEAD), D ** -0.5, 0.125, ((1, 4),))
    w_value = scatter_about(key_of[4], (D, HEADS * 2 * HEAD), D ** -0.5, 0.125, ((1, 4),))
    query_gain = jnp.clip(jax.random.uniform(key_of[5], (HEAD,), jnp.float32, 1.0, 1.8), 1.0, 1.8)
    key_gain = jnp.clip(jax.random.uniform(key_of[6], (HEAD,), jnp.float32, 1.0, 1.8), 1.0, 1.8)
    mix_lambda = jnp.clip(0.3 + 0.5 * jax.random.uniform(key_of[7], (HEADS,), jnp.float32) ** levels(key_of[7], (HEADS,), ((0, 4),), -0.2, 0.2), 0.3, 0.8)
    head_gain = jnp.clip(1.0 + 0.18 * jax.random.normal(key_of[8], (2 * HEAD,), jnp.float32), 0.1, 1.9)
    w_mix_out = scatter_about(key_of[9], (HEADS * 2 * HEAD, D), (HEADS * 2 * HEAD) ** -0.5, 0.125, ((1, 4),))
    x_exp = scatter_about(key_of[10], (TOKENS_B, D), 1.0, 6.0, ((0, 8),))
    exp_gain = jnp.clip(1.0 + 0.18 * jax.random.normal(key_of[11], (D,), jnp.float32), 0.1, 1.9)
    routes_keys = jax.random.split(jax.random.fold_in(key_of[12], 1), TOKENS_B // TOK_B)
    routes_turns = jax.random.permutation(jax.random.fold_in(key_of[12], 3), TOKENS_B // TOK_B)
    routes = jax.vmap(lambda own, number: assign_block(jax.random.fold_in(key_of[12], 2), own, number, TOK_B, EXPERTS, TOPK, CAP, 1))(routes_keys, routes_turns).reshape((TOKENS_B, TOPK))
    route_weight = jnp.clip(0.1 + 0.9 * jax.random.uniform(key_of[13], (TOKENS_B, TOPK), jnp.float32) ** levels(key_of[13], (TOKENS_B, TOPK), ((0, 8),), -0.2, 0.2), 0.1, 1.0)
    w_gate = scatter_about(key_of[14], (EXPERTS, D, FF), (D // 9) ** -0.5, 0.375, ((0, 8), (2, 4)))
    w_up = scatter_about(key_of[15], (EXPERTS, D, FF), (D // 9) ** -0.5, 0.375, ((0, 8), (2, 4)))
    w_down = scatter_about(key_of[16], (EXPERTS, FF, D), (FF * 16) ** -0.5, 0.03125, ((0, 8), (2, 4)))
    return dict(x_mix=x_mix, mix_gain=mix_gain, w_query=w_query, w_key=w_key, w_value=w_value, query_gain=query_gain, key_gain=key_gain, mix_lambda=mix_lambda, head_gain=head_gain, w_mix_out=w_mix_out, x_exp=x_exp, exp_gain=exp_gain, routes=routes, route_weight=route_weight, w_gate=w_gate, w_up=w_up, w_down=w_down)


def rms_rows(matrix, gain, epsilon):
    wide = matrix.astype(jnp.float32)
    return wide * lax.rsqrt(lax.optimization_barrier(jnp.mean(wide * wide, axis=-1, keepdims=True)) + epsilon) * gain

def to_float(rounded):
    return lax.optimization_barrier(rounded).astype(jnp.float32)

def slot_ids(chosen_rows, experts, capacity):
    flat_ids = chosen_rows.reshape(-1)
    onehot = (flat_ids[:, None] == jnp.arange(experts, dtype=jnp.int32)[None, :]).astype(jnp.int32)
    before = jnp.cumsum(onehot, axis=0) - onehot
    position = lax.optimization_barrier(jnp.sum(before * onehot, axis=1))
    return flat_ids * capacity + position

def attention_half(x_mix, mix_gain, w_query, w_key, w_value, query_gain, key_gain, mix_lambda, head_gain, w_mix_out):
    seq_len = x_mix.shape[0]
    normed = rms_rows(x_mix, mix_gain, 1e-05).astype(jnp.bfloat16)
    queries = jnp.dot(normed, w_query, preferred_element_type=jnp.float32).reshape(seq_len, HEADS, 2, HEAD)
    queries = (rms_rows(queries, query_gain, 1e-06) * HEAD ** (-0.5)).astype(jnp.bfloat16)
    key_rows = jnp.dot(normed, w_key, preferred_element_type=jnp.float32).reshape(seq_len, HEADS, 2, HEAD)
    key_rows = rms_rows(key_rows, key_gain, 1e-06).astype(jnp.bfloat16)
    values = jnp.dot(normed, w_value, preferred_element_type=jnp.float32).astype(jnp.bfloat16)
    values = values.reshape(seq_len, HEADS, 2 * HEAD)
    position = jnp.arange(seq_len, dtype=jnp.int32)
    visible = position[None, :] <= position[:, None]

    def one_head(operands):
        query_head, key_head, value_head, lambda_head = operands
        scores = jnp.einsum('cqd,ckd->cqk', to_float(query_head), to_float(key_head))
        weights_exp = jnp.where(visible[None], jnp.exp(scores), 0.0)
        denominator = lax.optimization_barrier(jnp.sum(weights_exp, axis=-1))
        numerator = jnp.einsum('cqk,kd->cqd', to_float(weights_exp.astype(jnp.bfloat16)), to_float(value_head))
        head_mix = numerator[0] / denominator[0][:, None] - lambda_head * numerator[1] / denominator[1][:, None]
        return (rms_rows(head_mix, head_gain, 1e-05) * 0.8).astype(jnp.bfloat16)
    outputs = lax.map(one_head, (queries.transpose(1, 2, 0, 3), key_rows.transpose(1, 2, 0, 3), values.transpose(1, 0, 2), mix_lambda))
    head_rows = outputs.transpose(1, 0, 2).reshape(seq_len, HEADS * 2 * HEAD)
    return jnp.dot(head_rows, w_mix_out, preferred_element_type=jnp.float32).astype(jnp.bfloat16)

def place_rows(slot_index, pair_rows):
    return jnp.zeros((EXPERTS * CAP,), jnp.int32).at[slot_index].set(pair_rows)

def mark_slots(slot_index):
    return jnp.zeros((EXPERTS * CAP,), jnp.bool_).at[slot_index].set(True)

def expert_half(x_exp, exp_gain, routes, route_weight, w_gate, w_up, w_down):
    blocks = N_EP
    normed = rms_rows(x_exp, exp_gain, 1e-05).astype(jnp.bfloat16).reshape(blocks, TOK_B, D)
    slot_index = jax.vmap(partial(slot_ids, experts=EXPERTS, capacity=CAP))(routes.reshape(blocks, TOK_B, TOPK))
    pair_rows = jnp.arange(TOK_B * TOPK, dtype=jnp.int32) // TOPK
    source = jax.vmap(partial(place_rows, pair_rows=pair_rows))(slot_index)
    filled = jax.vmap(mark_slots)(slot_index)
    pair_weight = route_weight.reshape(blocks, TOK_B * TOPK)

    def one_expert(running, expert):
        src_rows = lax.dynamic_slice_in_dim(source, expert * CAP, CAP, 1)
        full_slots = lax.dynamic_slice_in_dim(filled, expert * CAP, CAP, 1)
        inputs = jnp.take_along_axis(normed, src_rows[:, :, None], axis=1)
        inputs = jnp.where(full_slots[:, :, None], inputs, jnp.zeros_like(inputs)).reshape(blocks * CAP, D)
        gate_pre = jnp.dot(inputs, w_gate[expert], preferred_element_type=jnp.float32)
        up_pre = jnp.dot(inputs, w_up[expert], preferred_element_type=jnp.float32)
        gate_pre = jnp.minimum(gate_pre, 7.0)
        up_pre = jnp.clip(up_pre, -7.0, 7.0)
        hidden = (gate_pre * jax.nn.sigmoid(1.702 * gate_pre) * (up_pre + 1.0)).astype(jnp.bfloat16)
        result = jnp.dot(hidden, w_down[expert], preferred_element_type=jnp.float32).astype(jnp.bfloat16)
        result = result.reshape(blocks, CAP, D)
        chosen = slot_index // CAP == expert
        place_index = slot_index % CAP
        combine = jnp.where(chosen, pair_weight, 0.0)
        onehot = place_index[:, :, None] == jnp.arange(CAP, dtype=jnp.int32)[None, None, :]
        matrix = jnp.where(onehot, combine[:, :, None], 0.0)
        matrix = lax.optimization_barrier(jnp.sum(matrix.reshape(blocks, TOK_B, TOPK, CAP), axis=2))
        running = running + jnp.einsum('brc,bcd->brd', matrix, to_float(result), precision=lax.Precision.HIGHEST)
        return (running, None)
    start = jnp.zeros((blocks, TOK_B, D), jnp.float32)
    summed, unused = lax.scan(one_expert, start, jnp.arange(EXPERTS, dtype=jnp.int32))
    return summed.reshape(blocks * TOK_B, D).astype(jnp.bfloat16)

def reference(x_mix, mix_gain, w_query, w_key, w_value, query_gain, key_gain, mix_lambda, head_gain, w_mix_out, x_exp, exp_gain, routes, route_weight, w_gate, w_up, w_down):
    attn_out = attention_half(x_mix, mix_gain, w_query, w_key, w_value, query_gain, key_gain, mix_lambda, head_gain, w_mix_out)
    moe_out = expert_half(x_exp, exp_gain, routes, route_weight, w_gate, w_up, w_down)
    return (attn_out, moe_out)
```

```python
import functools
import jax
import jax.numpy as jnp
from jax import lax
from jax.experimental import pallas as pl
from jax.experimental.pallas import tpu as pltpu
from jax.sharding import PartitionSpec as P


def rms_rows(matrix, gain, epsilon):
    wide = matrix.astype(jnp.float32)
    return wide * lax.rsqrt(jnp.mean(wide * wide, axis=-1, keepdims=True) + epsilon) * gain


def kernel(
    n,
    parts,
    top,
    cap,
    head_size,
    q_ref,
    kv_ref,
    tok_ref,
    info_ref,
    lam_ref,
    hgain_ref,
    wout_ref,
    wgate_ref,
    wup_ref,
    wdown_ref,
    attn_ref,
    moe_ref,
    kv,
    tok,
    info,
    flat,
    hid,
    res,
    ret,
    numer,
    denom,
    heads,
    tok_s,
    tok_r,
    info_s,
    info_r,
    core_s,
    core_r,
    kv_s,
    kv_r,
    hid_s,
    hid_r,
    ret_s,
    ret_r,
    head_s,
    head_r,
):
    half = n // 2
    me = lax.axis_index("ep")
    mine = lax.axis_index("tp")
    odd = me % 2
    pos = (1 - odd) * (me // 2) + odd * (n - 1 - me // 2)

    def at(place):
        place = (place + 2 * n) % n
        high = place // half
        return (1 - high) * 2 * place + high * (2 * (n - 1 - place) + 1)

    right, left = at(pos + 1), at(pos - 1)
    core = mine % 2
    twin = mine + 1 - 2 * core
    rows_b, model = tok_ref.shape
    rows_a, pair_width = kv_ref.shape
    width = pair_width // 2
    side = model // 2
    local = wgate_ref.shape[1]
    f32, bf16 = jnp.float32, jnp.bfloat16

    barrier = pltpu.get_barrier_semaphore()
    for i in range(1, n):
        pl.semaphore_signal(
            barrier, inc=1, device_id={"ep": (me + i) % n}, device_id_type=pl.DeviceIdType.MESH
        )
    for i in range(1, parts):
        pl.semaphore_signal(
            barrier, inc=1, device_id={"tp": (mine + i) % parts}, device_id_type=pl.DeviceIdType.MESH
        )
    pl.semaphore_wait(barrier, n - 1 + parts - 1)

    def push(src, dst, s_sem, r_sem, where):
        return pltpu.make_async_remote_copy(
            src_ref=src,
            dst_ref=dst,
            send_sem=s_sem,
            recv_sem=r_sem,
            device_id=where,
            device_id_type=pl.DeviceIdType.MESH,
        )

    def span(step, way, rows):
        if step < half:
            return pl.ds(0, rows)
        return pl.ds(way * (rows // 2), rows // 2)

    def held(step, way):
        return at(pos - step) if way == 0 else at(pos + step)

    def tok_copies(step):
        out = []
        for way in (0, 1):
            where = {"ep": right if way == 0 else left}
            b = held(step - 1, way)
            cols = pl.ds(pl.multiple_of(core * side, side), side)
            rows = span(step, way, rows_b)
            if step == 1:
                src = tok_ref.at[rows, cols]
            else:
                src = tok.at[b, rows, cols]
            i = 2 * (step - 1) + way
            out.append(push(src, tok.at[b, rows, cols], tok_s.at[i], tok_r.at[i], where))
            if step < half or way == 0:
                src = info_ref if step == 1 else info.at[b]
                out.append(push(src, info.at[b], info_s.at[i], info_r.at[i], where))
        return out

    def kv_copies(step):
        out = []
        for way in (0, 1):
            where = {"ep": right if way == 0 else left}
            b = held(step - 1, way)
            rows = span(step, way, rows_a)
            src = kv_ref.at[rows] if step == 1 else kv.at[b, rows]
            i = 2 * (step - 1) + way
            out.append(push(src, kv.at[b, rows], kv_s.at[i], kv_r.at[i], where))
        return out

    def core_copies(step):
        out = []
        for way in (0, 1):
            b = held(step, way)
            cols = pl.ds(pl.multiple_of(core * side, side), side)
            ref = tok.at[b, span(step, way, rows_b), cols]
            i = 2 * (step - 1) + way
            out.append(push(ref, ref, core_s.at[i], core_r.at[i], {"tp": twin}))
        return out

    def start(copies):
        for copy in copies:
            copy.start()
        return copies

    def wait_recv(copies):
        for copy in copies:
            copy.wait_recv()

    def slot_block(slot):
        return held((slot + 1) // 2, (slot + 1) % 2)

    def slot_rows(block_info, expert):
        named = block_info[:top, :] == expert
        member = jnp.sum(named.astype(f32), axis=0, keepdims=True)
        row = lax.broadcasted_iota(jnp.int32, (rows_b, rows_b), 0)
        col = lax.broadcasted_iota(jnp.int32, (rows_b, rows_b), 1)
        earlier = (row < col).astype(bf16)
        spread = jnp.broadcast_to(member, (16, rows_b)).astype(bf16)
        before = jnp.dot(spread, earlier, preferred_element_type=f32)[:1]
        place = lax.broadcasted_iota(jnp.int32, (cap, rows_b), 0).astype(f32)
        return ((place == before) & (member > 0.0)).astype(f32).astype(bf16), named

    def compact(slot):
        if slot == 0:
            rows, notes = tok_ref[...], info_ref[...]
        else:
            b = slot_block(slot)
            rows, notes = tok[b], info[b]
        chosen, _ = slot_rows(notes, me.astype(f32))
        flat[slot * cap : (slot + 1) * cap, :] = jnp.dot(
            chosen, rows, preferred_element_type=f32
        ).astype(bf16)

    groups = 4
    per = n // groups
    size = per * cap
    tile = min(256, local)

    def hidden_group(g):
        for slot in range(g * per, (g + 1) * per):
            compact(slot)

        @pl.loop(0, local // tile)
        def _(c):
            cols = pl.ds(pl.multiple_of(c * tile, tile), tile)
            rows = flat[g * size : (g + 1) * size, :]
            gate = jnp.dot(rows, wgate_ref[:, cols], preferred_element_type=f32)
            up = jnp.dot(rows, wup_ref[:, cols], preferred_element_type=f32)
            gate = jnp.minimum(gate, 7.0)
            up = jnp.clip(up, -7.0, 7.0)
            value = gate * jax.nn.sigmoid(1.702 * gate) * (up + 1.0)
            hid[mine, g * size : (g + 1) * size, cols] = value.astype(bf16)

        out = []
        for i in range(1, parts):
            ref = hid.at[mine, pl.ds(g * size, size)]
            k = g * parts + i
            out.append(push(ref, ref, hid_s.at[k], hid_r.at[k], {"tp": (mine + i) % parts}))
        return start(out)

    def attend(k_of, diagonal):
        @pl.loop(0, width // (2 * head_size))
        def _(h):
            cols = pl.ds(pl.multiple_of(h * 2 * head_size, 2 * head_size), 2 * head_size)
            vcols = pl.ds(pl.multiple_of(width + h * 2 * head_size, 2 * head_size), 2 * head_size)
            query, key, value = q_ref[:, cols], k_of(cols), k_of(vcols)
            for c in (0, 1):
                part = slice(c * head_size, (c + 1) * head_size)
                scores = lax.dot_general(
                    query[:, part],
                    key[:, part],
                    (((1,), (1,)), ((), ())),
                    preferred_element_type=f32,
                )
                expo = jnp.exp(scores)
                if diagonal:
                    row = lax.broadcasted_iota(jnp.int32, expo.shape, 0)
                    col = lax.broadcasted_iota(jnp.int32, expo.shape, 1)
                    expo = jnp.where(col <= row, expo, 0.0)
                total = jnp.broadcast_to(
                    jnp.sum(expo, axis=1, keepdims=True), (rows_a, 128)
                )
                mixed = jnp.dot(expo.astype(bf16), value, preferred_element_type=f32)
                if diagonal:
                    numer[c, :, cols] = mixed
                    denom[c, h] = total
                else:
                    numer[c, :, cols] += mixed
                    denom[c, h] += total

    def attend_step(step):
        for way in (0, 1) if step < half else (0,):
            b = held(step, way)

            @pl.when(b < me)
            def _():
                attend(lambda cols: kv[b, :, cols], False)

    sent = []
    now = start(tok_copies(1))
    sent += now
    attend(lambda cols: kv_ref[:, cols], True)
    cores, hids, kv_now = [], [], None
    early = max(1, half - 1)
    for step in range(1, half + 1):
        wait_recv(now)
        if step < half:
            now = start(tok_copies(step + 1))
            sent += now
        if step == early:
            kv_now = start(kv_copies(1))
            sent += kv_now
        cores = start(core_copies(step))
        sent += cores
        wait_recv(cores)
        for g in range(groups):
            if (g * per + per) // 2 == step:
                hids += hidden_group(g)
    sent += hids

    moe_step = (half + 1) // 2
    for step in range(1, half + 1):
        wait_recv(kv_now)
        if step < half:
            kv_now = start(kv_copies(step + 1))
            sent += kv_now
        attend_step(step)
        if step == moe_step:
            wait_recv(hids)

            @pl.loop(0, groups)
            def _(g):
                rows = pl.ds(pl.multiple_of(g * size, size), size)
                total = jnp.zeros((size, moe_ref.shape[1]), f32)
                for t in range(parts):
                    total += jnp.dot(
                        hid[t, rows, :],
                        wdown_ref[t * local : (t + 1) * local, :],
                        preferred_element_type=f32,
                    )
                res[rows, :] = total.astype(bf16)

            ret[me] = res[0:cap, :]
            rets = []
            for slot in range(1, n):
                b = slot_block(slot)
                d = (slot + 1) // 2 if slot % 2 == 1 else n - slot // 2
                rets.append(
                    push(
                        res.at[pl.ds(slot * cap, cap)],
                        ret.at[me],
                        ret_s.at[d],
                        ret_r.at[d],
                        {"ep": b},
                    )
                )
            sent += start(rets)

    @pl.loop(0, width // (2 * head_size))
    def _(h):
        cols = pl.ds(pl.multiple_of(h * 2 * head_size, 2 * head_size), 2 * head_size)
        first = numer[0, :, cols] / denom[0, h][:, :1]
        second = numer[1, :, cols] / denom[1, h][:, :1]
        mix = first - lam_ref[h] * second
        heads[mine, :, cols] = (rms_rows(mix, hgain_ref[...], 1e-05) * 0.8).astype(bf16)

    outs = []
    for i in range(1, parts):
        ref = heads.at[mine]
        outs.append(push(ref, ref, head_s.at[i], head_r.at[i], {"tp": (mine + i) % parts}))
    sent += start(outs)

    wait_recv(rets)
    total = jnp.zeros(moe_ref.shape, f32)
    notes = info_ref[...]
    for e in range(n):
        chosen, named = slot_rows(notes, float(e))
        weight = jnp.sum(jnp.where(named, notes[top:, :], 0.0), axis=0, keepdims=True)
        picked = lax.dot_general(
            chosen, ret[e], (((0,), (0,)), ((), ())), preferred_element_type=f32
        )
        total += picked * weight.T
    moe_ref[...] = total.astype(bf16)

    wait_recv(outs)
    result = jnp.zeros(attn_ref.shape, f32)
    for t in range(parts):
        result += jnp.dot(
            heads[t], wout_ref[t * width : (t + 1) * width, :], preferred_element_type=f32
        )
    attn_ref[...] = result.astype(bf16)
    for copy in sent:
        copy.wait_send()


def body(
    x_mix,
    mix_gain,
    w_query,
    w_key,
    w_value,
    query_gain,
    key_gain,
    mix_lambda,
    head_gain,
    w_mix_out,
    x_exp,
    exp_gain,
    routes,
    route_weight,
    w_gate,
    w_up,
    w_down,
):
    n, parts = lax.axis_size("ep"), lax.axis_size("tp")
    rows_a = x_mix.shape[0]
    rows_b, model = x_exp.shape
    head_size = query_gain.shape[0]
    width = w_query.shape[1]
    local = w_gate.shape[2]
    out_width = w_down.shape[2]
    head_count = width // (2 * head_size)
    top = routes.shape[1]
    cap = 3 * rows_b * top // (2 * n)
    cap = -(-cap // 16) * 16
    f32, bf16 = jnp.float32, jnp.bfloat16
    normed = rms_rows(x_mix, mix_gain, 1e-05).astype(bf16)

    def split_norm(weights, gain, scale):
        out = jnp.dot(normed, weights, preferred_element_type=f32)
        out = out.reshape(rows_a, head_count * 2, head_size)
        return (rms_rows(out, gain, 1e-06) * scale).astype(bf16).reshape(rows_a, width)

    queries = split_norm(w_query, query_gain, head_size ** (-0.5))
    key_rows = split_norm(w_key, key_gain, 1.0)
    values = jnp.dot(normed, w_value, preferred_element_type=f32).astype(bf16)
    both = jnp.concatenate([key_rows, values], axis=1)
    rows = rms_rows(x_exp, exp_gain, 1e-05).astype(bf16)
    info = jnp.concatenate([routes.astype(f32), route_weight], axis=1).T
    vmem = pl.BlockSpec(memory_space=pltpu.VMEM)
    smem = pl.BlockSpec(memory_space=pltpu.SMEM)
    dma = pltpu.SemaphoreType.DMA
    groups = 4
    return pl.pallas_call(
        functools.partial(kernel, n, parts, top, cap, head_size),
        out_shape=(
            jax.ShapeDtypeStruct((rows_a, w_mix_out.shape[1]), bf16),
            jax.ShapeDtypeStruct((rows_b, out_width), bf16),
        ),
        in_specs=[vmem, vmem, vmem, vmem, smem, vmem, vmem, vmem, vmem, vmem],
        out_specs=(vmem, vmem),
        scratch_shapes=[
            pltpu.VMEM((n, rows_a, 2 * width), bf16),
            pltpu.VMEM((n, rows_b, model), bf16),
            pltpu.VMEM((n, 2 * top, rows_b), f32),
            pltpu.VMEM((n * cap, model), bf16),
            pltpu.VMEM((parts, n * cap, local), bf16),
            pltpu.VMEM((n * cap, out_width), bf16),
            pltpu.VMEM((n, cap, out_width), bf16),
            pltpu.VMEM((2, rows_a, width), f32),
            pltpu.VMEM((2, head_count, rows_a, 128), f32),
            pltpu.VMEM((parts, rows_a, width), bf16),
            dma((n,)),
            dma((n,)),
            dma((n,)),
            dma((n,)),
            dma((n,)),
            dma((n,)),
            dma((n,)),
            dma((n,)),
            dma((groups * parts,)),
            dma((groups * parts,)),
            dma((n,)),
            dma((n,)),
            dma((parts,)),
            dma((parts,)),
        ],
        compiler_params=pltpu.CompilerParams(
            collective_id=0, has_side_effects=True, vmem_limit_bytes=60 * 1024 * 1024
        ),
    )(
        queries,
        both,
        rows,
        info,
        mix_lambda,
        head_gain.reshape(1, -1),
        w_mix_out,
        w_gate[0],
        w_up[0],
        w_down[0],
    )


def solution(mesh):
    return jax.shard_map(
        body,
        mesh=mesh,
        in_specs=(
            P("ep", None),
            P(),
            P(None, "tp"),
            P(None, "tp"),
            P(None, "tp"),
            P(),
            P(),
            P("tp"),
            P(),
            P(None, "tp"),
            P("ep", None),
            P(),
            P("ep", None),
            P("ep", None),
            P("ep", None, "tp"),
            P("ep", None, "tp"),
            P("ep", None, "tp"),
        ),
        out_specs=(P("ep", "tp"), P("ep", "tp")),
        check_vma=False,
    )
```

```python
import functools
import jax
import jax.numpy as jnp
from jax import lax
from jax.experimental import pallas as pl
from jax.experimental.pallas import tpu as pltpu
from jax.sharding import PartitionSpec as P


def rms_rows(matrix, gain, epsilon):
    wide = matrix.astype(jnp.float32)
    return wide * lax.rsqrt(jnp.mean(wide * wide, axis=-1, keepdims=True) + epsilon) * gain


def kernel(
    n,
    parts,
    top,
    cap,
    head_size,
    x_ref,
    xgain_ref,
    e_ref,
    egain_ref,
    gains_ref,
    info_ref,
    lam_ref,
    hgain_ref,
    wq_any,
    wk_any,
    wv_any,
    wgate_any,
    wup_any,
    wdown_any,
    wout_any,
    attn_ref,
    moe_ref,
    wq_ref,
    wk_ref,
    wv_ref,
    wgate_ref,
    wup_ref,
    wdown_ref,
    wout_ref,
    load_s,
    normed,
    q_ref,
    kv_ref,
    tok_ref,
    kv,
    tok,
    info,
    flat,
    hid,
    res,
    ret,
    numer,
    denom,
    heads,
    tok_s,
    tok_r,
    info_s,
    info_r,
    core_s,
    core_r,
    kv_s,
    kv_r,
    hid_s,
    hid_r,
    ret_s,
    ret_r,
    head_s,
    head_r,
):
    half = n // 2
    me = lax.axis_index("ep")
    mine = lax.axis_index("tp")
    odd = me % 2
    pos = (1 - odd) * (me // 2) + odd * (n - 1 - me // 2)

    def at(place):
        place = (place + 2 * n) % n
        high = place // half
        return (1 - high) * 2 * place + high * (2 * (n - 1 - place) + 1)

    right, left = at(pos + 1), at(pos - 1)
    core = mine % 2
    twin = mine + 1 - 2 * core
    rows_b, model = tok_ref.shape
    rows_a, pair_width = kv_ref.shape
    width = pair_width // 2
    side = model // 2
    local = wgate_ref.shape[1]
    f32, bf16 = jnp.float32, jnp.bfloat16

    loads = [
        pltpu.make_async_copy(source, target, load_s.at[i])
        for i, (source, target) in enumerate(
            (
                (wq_any, wq_ref),
                (wk_any, wk_ref),
                (wv_any, wv_ref),
                (wgate_any.at[0], wgate_ref),
                (wup_any.at[0], wup_ref),
                (wdown_any.at[0], wdown_ref),
                (wout_any, wout_ref),
            )
        )
    ]
    for load in loads:
        load.start()
    barrier = pltpu.get_barrier_semaphore()
    for i in range(1, n):
        pl.semaphore_signal(
            barrier, inc=1, device_id={"ep": (me + i) % n}, device_id_type=pl.DeviceIdType.MESH
        )
    for i in range(1, parts):
        pl.semaphore_signal(
            barrier, inc=1, device_id={"tp": (mine + i) % parts}, device_id_type=pl.DeviceIdType.MESH
        )
    tok_ref[...] = rms_rows(e_ref[...], egain_ref[...], 1e-05).astype(bf16)
    pl.semaphore_wait(barrier, n - 1 + parts - 1)

    def push(src, dst, s_sem, r_sem, where):
        return pltpu.make_async_remote_copy(
            src_ref=src,
            dst_ref=dst,
            send_sem=s_sem,
            recv_sem=r_sem,
            device_id=where,
            device_id_type=pl.DeviceIdType.MESH,
        )

    def span(step, way, rows):
        if step < half:
            return pl.ds(0, rows)
        return pl.ds(way * (rows // 2), rows // 2)

    def held(step, way):
        return at(pos - step) if way == 0 else at(pos + step)

    def tok_copies(step, piece):
        out = []
        for way in (0, 1):
            where = {"ep": right if way == 0 else left}
            b = held(step - 1, way)
            cols = pl.ds(pl.multiple_of(core * side + piece * (side // 2), side // 2), side // 2)
            rows = span(step, way, rows_b)
            if step == 1:
                src = tok_ref.at[rows, cols]
            else:
                src = tok.at[b, rows, cols]
            i = 2 * (step - 1) + way
            j = piece * n + i
            out.append(push(src, tok.at[b, rows, cols], tok_s.at[j], tok_r.at[j], where))
            if piece == 0 and (step < half or way == 0):
                src = info_ref if step == 1 else info.at[b]
                out.append(push(src, info.at[b], info_s.at[i], info_r.at[i], where))
        return out

    def kv_copies(step, piece):
        out = []
        for way in (0, 1):
            where = {"ep": right if way == 0 else left}
            b = held(step - 1, way)
            rows = span(step, way, rows_a)
            cols = pl.ds(piece * width, width)
            src = kv_ref.at[rows, cols] if step == 1 else kv.at[b, rows, cols]
            i = 2 * (step - 1) + way + piece * n
            out.append(push(src, kv.at[b, rows, cols], kv_s.at[i], kv_r.at[i], where))
        return out

    def core_copies(step, piece):
        out = []
        for way in (0, 1):
            b = held(step, way)
            cols = pl.ds(pl.multiple_of(core * side + piece * (side // 2), side // 2), side // 2)
            ref = tok.at[b, span(step, way, rows_b), cols]
            i = 2 * (step - 1) + way + piece * n
            out.append(push(ref, ref, core_s.at[i], core_r.at[i], {"tp": twin}))
        return out

    def start(copies):
        for copy in copies:
            copy.start()
        return copies

    def wait_recv(copies):
        for copy in copies:
            copy.wait_recv()

    def slot_block(slot):
        return held((slot + 1) // 2, (slot + 1) % 2)

    def slot_rows(block_info, expert):
        named = block_info[:top, :] == expert
        member = jnp.sum(named.astype(f32), axis=0, keepdims=True)
        row = lax.broadcasted_iota(jnp.int32, (rows_b, rows_b), 0)
        col = lax.broadcasted_iota(jnp.int32, (rows_b, rows_b), 1)
        earlier = (row < col).astype(bf16)
        spread = jnp.broadcast_to(member, (16, rows_b)).astype(bf16)
        before = jnp.dot(spread, earlier, preferred_element_type=f32)[:1]
        place = lax.broadcasted_iota(jnp.int32, (cap, rows_b), 0).astype(f32)
        return ((place == before) & (member > 0.0)).astype(f32).astype(bf16), named

    def compact(slot):
        if slot == 0:
            rows, notes = tok_ref[...], info_ref[...]
        else:
            b = slot_block(slot)
            rows, notes = tok[b], info[b]
        chosen, _ = slot_rows(notes, me.astype(f32))
        flat[slot * cap : (slot + 1) * cap, :] = jnp.dot(
            chosen, rows, preferred_element_type=f32
        ).astype(bf16)

    groups = 4
    per = n // groups
    size = per * cap
    tile = min(256, local)

    def hidden_group(g):
        for slot in range(g * per, (g + 1) * per):
            compact(slot)

        @pl.loop(0, local // tile)
        def _(c):
            cols = pl.ds(pl.multiple_of(c * tile, tile), tile)
            rows = flat[g * size : (g + 1) * size, :]
            gate = jnp.dot(rows, wgate_ref[:, cols], preferred_element_type=f32)
            up = jnp.dot(rows, wup_ref[:, cols], preferred_element_type=f32)
            gate = jnp.minimum(gate, 7.0)
            up = jnp.clip(up, -7.0, 7.0)
            value = gate * jax.nn.sigmoid(1.702 * gate) * (up + 1.0)
            hid[mine, g * size : (g + 1) * size, cols] = value.astype(bf16)

    def hid_ref(owner, g):
        return hid.at[owner, pl.ds(g * size, size)]

    def head_ref(owner, g):
        return heads.at[owner]

    def exchange(ref_of, g, sems):
        out = []
        for i in range(0, parts, 2):
            k = g * parts + i
            ref = ref_of(mine, g)
            if i == 0:
                out.append(push(ref, ref, sems[0].at[k], sems[1].at[k], {"tp": twin}))
            else:
                where = {"tp": (mine + i) % parts}
                out.append(push(ref, ref, sems[0].at[k], sems[1].at[k], where))
        return start(out)

    def relay(ref_of, g, sems, firsts):
        out = []
        for i in range(2, parts, 2):
            firsts[i // 2].wait_recv()
            k = g * parts + i + 1
            ref = ref_of((mine + parts - i) % parts, g)
            out.append(push(ref, ref, sems[0].at[k], sems[1].at[k], {"tp": twin}))
        return start(out)

    def attend(k_of, diagonal):
        @pl.loop(0, width // (2 * head_size))
        def _(h):
            cols = pl.ds(pl.multiple_of(h * 2 * head_size, 2 * head_size), 2 * head_size)
            vcols = pl.ds(pl.multiple_of(width + h * 2 * head_size, 2 * head_size), 2 * head_size)
            query, key, value = q_ref[:, cols], k_of(cols), k_of(vcols)
            for c in (0, 1):
                part = slice(c * head_size, (c + 1) * head_size)
                scores = lax.dot_general(
                    query[:, part],
                    key[:, part],
                    (((1,), (1,)), ((), ())),
                    preferred_element_type=f32,
                )
                expo = jnp.exp(scores)
                if diagonal:
                    row = lax.broadcasted_iota(jnp.int32, expo.shape, 0)
                    col = lax.broadcasted_iota(jnp.int32, expo.shape, 1)
                    expo = jnp.where(col <= row, expo, 0.0)
                total = jnp.broadcast_to(
                    jnp.sum(expo, axis=1, keepdims=True), (rows_a, 128)
                )
                mixed = jnp.dot(expo.astype(bf16), value, preferred_element_type=f32)
                if diagonal:
                    numer[c, :, cols] = mixed
                    denom[c, h] = total
                else:
                    numer[c, :, cols] += mixed
                    denom[c, h] += total

    def attend_step(step):
        for way in (0, 1) if step < half else (0,):
            b = held(step, way)

            @pl.when(b < me)
            def _():
                attend(lambda cols: kv[b, :, cols], False)

    sent = []
    now = [start(tok_copies(1, piece)) for piece in (0, 1)]
    sent += now[0] + now[1]
    normed[...] = rms_rows(x_ref[...], xgain_ref[...], 1e-05).astype(bf16)
    for load in loads[:3]:
        load.wait()
    wide = gains_ref.shape[1]

    @pl.loop(0, width // wide)
    def _(t):
        cols = pl.ds(pl.multiple_of(t * wide, wide), wide)
        vcols = pl.ds(pl.multiple_of(width + t * wide, wide), wide)
        group = lax.broadcasted_iota(jnp.int32, (rows_a, wide), 1) // head_size

        def unit(weights, gain):
            out = jnp.dot(normed[...], weights[:, cols], preferred_element_type=f32)
            square = out * out
            factor = jnp.zeros_like(out)
            for g in range(wide // head_size):
                here = group == g
                mean = jnp.sum(jnp.where(here, square, 0.0), axis=1, keepdims=True) / head_size
                factor = jnp.where(here, lax.rsqrt(mean + 1e-06), factor)
            return out * factor * gain

        q_ref[:, cols] = (unit(wq_ref, gains_ref[0:1, :]) * head_size ** (-0.5)).astype(bf16)
        kv_ref[:, cols] = unit(wk_ref, gains_ref[1:2, :]).astype(bf16)
        kv_ref[:, vcols] = jnp.dot(
            normed[...], wv_ref[:, cols], preferred_element_type=f32
        ).astype(bf16)

    for load in loads[3:5]:
        load.wait()
    hid_sems, head_sems = (hid_s, hid_r), (head_s, head_r)
    hids, relays, kv_now = [], [], None
    early = max(1, half - 1)
    for step in range(1, half + 1):
        cores, later = [], []
        for piece in (0, 1):
            wait_recv(now[piece])
            if step < half:
                later.append(start(tok_copies(step + 1, piece)))
                sent += later[-1]
            cores += start(core_copies(step, piece))
        sent += cores
        now = later
        if step == early:
            kv_now = [start(kv_copies(1, piece)) for piece in (0, 1)]
            sent += kv_now[0] + kv_now[1]
        if step == 1:
            attend(lambda cols: kv_ref[:, cols], True)
        if hids:
            relays += relay(hid_ref, len(hids) - 1, hid_sems, hids[-1])
        wait_recv(cores)
        for g in range(groups):
            if (g * per + per) // 2 == step:
                hidden_group(g)
                hids.append(exchange(hid_ref, g, hid_sems))

    moe_step = (half + 1) // 2
    for step in range(1, half + 1):
        later = []
        for piece in (0, 1):
            wait_recv(kv_now[piece])
            if step < half:
                later.append(start(kv_copies(step + 1, piece)))
                sent += later[-1]
        kv_now = later
        if step == 1:
            relays += relay(hid_ref, groups - 1, hid_sems, hids[-1])
        if step == moe_step:
            loads[5].wait()
            for copies in hids:
                copies[0].wait_recv()
            wait_recv(relays)

            @pl.loop(0, groups)
            def _(g):
                rows = pl.ds(pl.multiple_of(g * size, size), size)
                total = jnp.zeros((size, moe_ref.shape[1]), f32)
                for t in range(parts):
                    total += jnp.dot(
                        hid[t, rows, :],
                        wdown_ref[t * local : (t + 1) * local, :],
                        preferred_element_type=f32,
                    )
                res[rows, :] = total.astype(bf16)

            ret[me] = res[0:cap, :]
            rets = []
            for slot in range(1, n):
                b = slot_block(slot)
                d = (slot + 1) // 2 if slot % 2 == 1 else n - slot // 2
                rets.append(
                    push(
                        res.at[pl.ds(slot * cap, cap)],
                        ret.at[me],
                        ret_s.at[d],
                        ret_r.at[d],
                        {"ep": b},
                    )
                )
            sent += start(rets)
        attend_step(step)

    @pl.loop(0, width // (2 * head_size))
    def _(h):
        cols = pl.ds(pl.multiple_of(h * 2 * head_size, 2 * head_size), 2 * head_size)
        first = numer[0, :, cols] / denom[0, h][:, :1]
        second = numer[1, :, cols] / denom[1, h][:, :1]
        mix = first - lam_ref[h] * second
        heads[mine, :, cols] = (rms_rows(mix, hgain_ref[...], 1e-05) * 0.8).astype(bf16)

    outs = exchange(head_ref, 0, head_sems)
    passed = relay(head_ref, 0, head_sems, outs)
    for copies in hids:
        sent += copies
    sent += relays + outs + passed

    wait_recv(rets)
    total = jnp.zeros(moe_ref.shape, f32)
    notes = info_ref[...]
    for e in range(n):
        chosen, named = slot_rows(notes, float(e))
        weight = jnp.sum(jnp.where(named, notes[top:, :], 0.0), axis=0, keepdims=True)
        picked = lax.dot_general(
            chosen, ret[e], (((0,), (0,)), ((), ())), preferred_element_type=f32
        )
        total += picked * weight.T
    moe_ref[...] = total.astype(bf16)

    loads[6].wait()
    outs[0].wait_recv()
    wait_recv(passed)
    result = jnp.zeros(attn_ref.shape, f32)
    for t in range(parts):
        result += jnp.dot(
            heads[t], wout_ref[t * width : (t + 1) * width, :], preferred_element_type=f32
        )
    attn_ref[...] = result.astype(bf16)
    for copy in sent:
        copy.wait_send()


def body(
    x_mix,
    mix_gain,
    w_query,
    w_key,
    w_value,
    query_gain,
    key_gain,
    mix_lambda,
    head_gain,
    w_mix_out,
    x_exp,
    exp_gain,
    routes,
    route_weight,
    w_gate,
    w_up,
    w_down,
):
    n, parts = lax.axis_size("ep"), lax.axis_size("tp")
    rows_a = x_mix.shape[0]
    rows_b, model = x_exp.shape
    head_size = query_gain.shape[0]
    width = w_query.shape[1]
    local = w_gate.shape[2]
    out_width = w_down.shape[2]
    head_count = width // (2 * head_size)
    top = routes.shape[1]
    cap = 3 * rows_b * top // (2 * n)
    cap = -(-cap // 16) * 16
    f32, bf16 = jnp.float32, jnp.bfloat16
    wide = min(256, width)
    gains = jnp.tile(jnp.stack([query_gain, key_gain]), (1, wide // head_size))
    info = jnp.concatenate([routes.astype(f32), route_weight], axis=1).T
    vmem = pl.BlockSpec(memory_space=pltpu.VMEM)
    smem = pl.BlockSpec(memory_space=pltpu.SMEM)
    hbm = pl.BlockSpec(memory_space=pl.ANY)
    dma = pltpu.SemaphoreType.DMA
    groups = 4
    return pl.pallas_call(
        functools.partial(kernel, n, parts, top, cap, head_size),
        out_shape=(
            jax.ShapeDtypeStruct((rows_a, w_mix_out.shape[1]), bf16),
            jax.ShapeDtypeStruct((rows_b, out_width), bf16),
        ),
        in_specs=[vmem] * 6 + [smem, vmem] + [hbm] * 7,
        out_specs=(vmem, vmem),
        scratch_shapes=[
            pltpu.VMEM(w_query.shape, bf16),
            pltpu.VMEM(w_key.shape, bf16),
            pltpu.VMEM(w_value.shape, bf16),
            pltpu.VMEM(w_gate.shape[1:], bf16),
            pltpu.VMEM(w_up.shape[1:], bf16),
            pltpu.VMEM(w_down.shape[1:], bf16),
            pltpu.VMEM(w_mix_out.shape, bf16),
            dma((7,)),
            pltpu.VMEM((rows_a, model), bf16),
            pltpu.VMEM((rows_a, width), bf16),
            pltpu.VMEM((rows_a, 2 * width), bf16),
            pltpu.VMEM((rows_b, model), bf16),
            pltpu.VMEM((n, rows_a, 2 * width), bf16),
            pltpu.VMEM((n, rows_b, model), bf16),
            pltpu.VMEM((n, 2 * top, rows_b), f32),
            pltpu.VMEM((n * cap, model), bf16),
            pltpu.VMEM((parts, n * cap, local), bf16),
            pltpu.VMEM((n * cap, out_width), bf16),
            pltpu.VMEM((n, cap, out_width), bf16),
            pltpu.VMEM((2, rows_a, width), f32),
            pltpu.VMEM((2, head_count, rows_a, 128), f32),
            pltpu.VMEM((parts, rows_a, width), bf16),
            dma((2 * n,)),
            dma((2 * n,)),
            dma((n,)),
            dma((n,)),
            dma((2 * n,)),
            dma((2 * n,)),
            dma((2 * n,)),
            dma((2 * n,)),
            dma((groups * parts,)),
            dma((groups * parts,)),
            dma((n,)),
            dma((n,)),
            dma((parts,)),
            dma((parts,)),
        ],
        compiler_params=pltpu.CompilerParams(
            collective_id=0, has_side_effects=True, vmem_limit_bytes=60 * 1024 * 1024
        ),
    )(
        x_mix,
        mix_gain.reshape(1, -1),
        x_exp,
        exp_gain.reshape(1, -1),
        gains,
        info,
        mix_lambda,
        head_gain.reshape(1, -1),
        w_query,
        w_key,
        w_value,
        w_gate,
        w_up,
        w_down,
        w_mix_out,
    )


def solution(mesh):
    return jax.shard_map(
        body,
        mesh=mesh,
        in_specs=(
            P("ep", None),
            P(),
            P(None, "tp"),
            P(None, "tp"),
            P(None, "tp"),
            P(),
            P(),
            P("tp"),
            P(),
            P(None, "tp"),
            P("ep", None),
            P(),
            P("ep", None),
            P("ep", None),
            P("ep", None, "tp"),
            P("ep", None, "tp"),
            P("ep", None, "tp"),
        ),
        out_specs=(P("ep", "tp"), P("ep", "tp")),
        check_vma=False,
    )
```

```python
import functools
import jax
import jax.numpy as jnp
from jax import lax
from jax.experimental import pallas as pl
from jax.experimental.pallas import tpu as pltpu
from jax.sharding import PartitionSpec as P


def rms_rows(matrix, gain, epsilon):
    wide = matrix.astype(jnp.float32)
    return wide * lax.rsqrt(jnp.mean(wide * wide, axis=-1, keepdims=True) + epsilon) * gain


def kernel(
    n,
    parts,
    top,
    cap,
    head_size,
    x_ref,
    xgain_ref,
    e_ref,
    egain_ref,
    gains_ref,
    info_ref,
    lam_ref,
    hgain_ref,
    wq_any,
    wk_any,
    wv_any,
    wgate_any,
    wup_any,
    wdown_any,
    wout_any,
    attn_ref,
    moe_ref,
    wq_ref,
    wk_ref,
    wv_ref,
    wgate_ref,
    wup_ref,
    wdown_ref,
    wout_ref,
    load_s,
    normed,
    q_ref,
    kv_ref,
    tok_ref,
    kv,
    tok,
    info,
    flat,
    hid,
    res,
    ret,
    numer,
    denom,
    heads,
    tok_s,
    tok_r,
    info_s,
    info_r,
    core_s,
    core_r,
    kv_s,
    kv_r,
    hid_s,
    hid_r,
    ret_s,
    ret_r,
    head_s,
    head_r,
):
    half = n // 2
    me = lax.axis_index("ep")
    mine = lax.axis_index("tp")
    odd = me % 2
    pos = (1 - odd) * (me // 2) + odd * (n - 1 - me // 2)

    def at(place):
        place = (place + 2 * n) % n
        high = place // half
        return (1 - high) * 2 * place + high * (2 * (n - 1 - place) + 1)

    right, left = at(pos + 1), at(pos - 1)
    core = mine % 2
    twin = mine + 1 - 2 * core
    rows_b, model = tok_ref.shape
    rows_a, pair_width = kv_ref.shape
    width = pair_width // 2
    side = model // 2
    local = wgate_ref.shape[1]
    f32, bf16 = jnp.float32, jnp.bfloat16

    loads = [
        pltpu.make_async_copy(source, target, load_s.at[i])
        for i, (source, target) in enumerate(
            (
                (wq_any, wq_ref),
                (wk_any, wk_ref),
                (wv_any, wv_ref),
                (wgate_any.at[0], wgate_ref),
                (wup_any.at[0], wup_ref),
                (wdown_any.at[0], wdown_ref),
                (wout_any, wout_ref),
            )
        )
    ]
    for load in loads:
        load.start()
    barrier = pltpu.get_barrier_semaphore()
    for i in range(1, n):
        pl.semaphore_signal(
            barrier, inc=1, device_id={"ep": (me + i) % n}, device_id_type=pl.DeviceIdType.MESH
        )
    for i in range(1, parts):
        pl.semaphore_signal(
            barrier, inc=1, device_id={"tp": (mine + i) % parts}, device_id_type=pl.DeviceIdType.MESH
        )
    tok_ref[...] = rms_rows(e_ref[...], egain_ref[...], 1e-05).astype(bf16)
    pl.semaphore_wait(barrier, n - 1 + parts - 1)

    def push(src, dst, s_sem, r_sem, where):
        return pltpu.make_async_remote_copy(
            src_ref=src,
            dst_ref=dst,
            send_sem=s_sem,
            recv_sem=r_sem,
            device_id=where,
            device_id_type=pl.DeviceIdType.MESH,
        )

    def span(step, way, rows):
        if step < half:
            return pl.ds(0, rows)
        return pl.ds(way * (rows // 2), rows // 2)

    def held(step, way):
        return at(pos - step) if way == 0 else at(pos + step)

    def tok_copies(step, piece):
        out = []
        for way in (0, 1):
            where = {"ep": right if way == 0 else left}
            b = held(step - 1, way)
            cols = pl.ds(pl.multiple_of(core * side + piece * (side // 2), side // 2), side // 2)
            rows = span(step, way, rows_b)
            if step == 1:
                src = tok_ref.at[rows, cols]
            else:
                src = tok.at[b, rows, cols]
            i = 2 * (step - 1) + way
            j = piece * n + i
            out.append(push(src, tok.at[b, rows, cols], tok_s.at[j], tok_r.at[j], where))
            if piece == 0 and (step < half or way == 0):
                src = info_ref if step == 1 else info.at[b]
                out.append(push(src, info.at[b], info_s.at[i], info_r.at[i], where))
        return out

    def kv_copies(step, piece):
        out = []
        for way in (0, 1):
            where = {"ep": right if way == 0 else left}
            b = held(step - 1, way)
            rows = span(step, way, rows_a)
            cols = pl.ds(piece * width, width)
            src = kv_ref.at[rows, cols] if step == 1 else kv.at[b, rows, cols]
            i = 2 * (step - 1) + way + piece * n
            out.append(push(src, kv.at[b, rows, cols], kv_s.at[i], kv_r.at[i], where))
        return out

    def core_copies(step, piece):
        out = []
        for way in (0, 1):
            b = held(step, way)
            cols = pl.ds(pl.multiple_of(core * side + piece * (side // 2), side // 2), side // 2)
            ref = tok.at[b, span(step, way, rows_b), cols]
            i = 2 * (step - 1) + way + piece * n
            out.append(push(ref, ref, core_s.at[i], core_r.at[i], {"tp": twin}))
        return out

    def start(copies):
        for copy in copies:
            copy.start()
        return copies

    def wait_recv(copies):
        for copy in copies:
            copy.wait_recv()

    def slot_block(slot):
        return held((slot + 1) // 2, (slot + 1) % 2)

    def slot_rows(block_info, expert):
        named = block_info[:top, :] == expert
        member = jnp.sum(named.astype(f32), axis=0, keepdims=True)
        row = lax.broadcasted_iota(jnp.int32, (rows_b, rows_b), 0)
        col = lax.broadcasted_iota(jnp.int32, (rows_b, rows_b), 1)
        earlier = (row < col).astype(bf16)
        spread = jnp.broadcast_to(member, (16, rows_b)).astype(bf16)
        before = jnp.dot(spread, earlier, preferred_element_type=f32)[:1]
        place = lax.broadcasted_iota(jnp.int32, (cap, rows_b), 0).astype(f32)
        return ((place == before) & (member > 0.0)).astype(f32).astype(bf16), named

    def compact(slot):
        if slot == 0:
            rows, notes = tok_ref[...], info_ref[...]
        else:
            b = slot_block(slot)
            rows, notes = tok[b], info[b]
        chosen, _ = slot_rows(notes, me.astype(f32))
        flat[slot * cap : (slot + 1) * cap, :] = jnp.dot(
            chosen, rows, preferred_element_type=f32
        ).astype(bf16)

    groups = 4
    per = n // groups
    size = per * cap
    tile = min(256, local)

    def hidden_group(g):
        for slot in range(g * per, (g + 1) * per):
            compact(slot)

        @pl.loop(0, local // tile)
        def _(c):
            cols = pl.ds(pl.multiple_of(c * tile, tile), tile)
            rows = flat[g * size : (g + 1) * size, :]
            gate = jnp.dot(rows, wgate_ref[:, cols], preferred_element_type=f32)
            up = jnp.dot(rows, wup_ref[:, cols], preferred_element_type=f32)
            gate = jnp.minimum(gate, 7.0)
            up = jnp.clip(up, -7.0, 7.0)
            value = gate * jax.nn.sigmoid(1.702 * gate) * (up + 1.0)
            hid[mine, g * size : (g + 1) * size, cols] = value.astype(bf16)

    def hid_ref(owner, g):
        return hid.at[owner, pl.ds(g * size, size)]

    def head_ref(owner, g):
        return heads.at[owner]

    def exchange(ref_of, g, sems):
        out = []
        for i in range(0, parts, 2):
            k = g * parts + i
            ref = ref_of(mine, g)
            if i == 0:
                out.append(push(ref, ref, sems[0].at[k], sems[1].at[k], {"tp": twin}))
            else:
                where = {"tp": (mine + i) % parts}
                out.append(push(ref, ref, sems[0].at[k], sems[1].at[k], where))
        return start(out)

    def relay(ref_of, g, sems, firsts):
        out = []
        for i in range(2, parts, 2):
            firsts[i // 2].wait_recv()
            k = g * parts + i + 1
            ref = ref_of((mine + parts - i) % parts, g)
            out.append(push(ref, ref, sems[0].at[k], sems[1].at[k], {"tp": twin}))
        return start(out)

    def attend(k_of, diagonal):
        @pl.loop(0, width // (2 * head_size))
        def _(h):
            cols = pl.ds(pl.multiple_of(h * 2 * head_size, 2 * head_size), 2 * head_size)
            vcols = pl.ds(pl.multiple_of(width + h * 2 * head_size, 2 * head_size), 2 * head_size)
            query, key, value = q_ref[:, cols], k_of(cols), k_of(vcols)
            for c in (0, 1):
                part = slice(c * head_size, (c + 1) * head_size)
                scores = lax.dot_general(
                    query[:, part],
                    key[:, part],
                    (((1,), (1,)), ((), ())),
                    preferred_element_type=f32,
                )
                expo = jnp.exp(scores)
                if diagonal:
                    row = lax.broadcasted_iota(jnp.int32, expo.shape, 0)
                    col = lax.broadcasted_iota(jnp.int32, expo.shape, 1)
                    expo = jnp.where(col <= row, expo, 0.0)
                total = jnp.broadcast_to(
                    jnp.sum(expo, axis=1, keepdims=True), (rows_a, 128)
                )
                mixed = jnp.dot(expo.astype(bf16), value, preferred_element_type=f32)
                if diagonal:
                    numer[c, :, cols] = mixed
                    denom[c, h] = total
                else:
                    numer[c, :, cols] += mixed
                    denom[c, h] += total

    def attend_step(step):
        for way in (0, 1) if step < half else (0,):
            b = held(step, way)

            @pl.when(b < me)
            def _():
                attend(lambda cols: kv[b, :, cols], False)

    sent = []
    now = [start(tok_copies(1, piece)) for piece in (0, 1)]
    sent += now[0] + now[1]
    normed[...] = rms_rows(x_ref[...], xgain_ref[...], 1e-05).astype(bf16)
    for load in loads[:3]:
        load.wait()
    wide = gains_ref.shape[1]

    @pl.loop(0, width // wide)
    def _(t):
        cols = pl.ds(pl.multiple_of(t * wide, wide), wide)
        vcols = pl.ds(pl.multiple_of(width + t * wide, wide), wide)
        group = lax.broadcasted_iota(jnp.int32, (rows_a, wide), 1) // head_size

        def unit(weights, gain):
            out = jnp.dot(normed[...], weights[:, cols], preferred_element_type=f32)
            square = out * out
            factor = jnp.zeros_like(out)
            for g in range(wide // head_size):
                here = group == g
                mean = jnp.sum(jnp.where(here, square, 0.0), axis=1, keepdims=True) / head_size
                factor = jnp.where(here, lax.rsqrt(mean + 1e-06), factor)
            return out * factor * gain

        q_ref[:, cols] = (unit(wq_ref, gains_ref[0:1, :]) * head_size ** (-0.5)).astype(bf16)
        kv_ref[:, cols] = unit(wk_ref, gains_ref[1:2, :]).astype(bf16)
        kv_ref[:, vcols] = jnp.dot(
            normed[...], wv_ref[:, cols], preferred_element_type=f32
        ).astype(bf16)

    for load in loads[3:5]:
        load.wait()
    hid_sems, head_sems = (hid_s, hid_r), (head_s, head_r)
    hids, relays, kv_now = [], [], None
    early = max(1, half - 2)
    for step in range(1, half + 1):
        cores, later = [], []
        for piece in (0, 1):
            wait_recv(now[piece])
            if step < half:
                later.append(start(tok_copies(step + 1, piece)))
                sent += later[-1]
            cores += start(core_copies(step, piece))
        sent += cores
        now = later
        if step == early:
            kv_now = [start(kv_copies(1, piece)) for piece in (0, 1)]
            sent += kv_now[0] + kv_now[1]
        if step == 1:
            attend(lambda cols: kv_ref[:, cols], True)
        if hids:
            relays += relay(hid_ref, len(hids) - 1, hid_sems, hids[-1])
        wait_recv(cores)
        for g in range(groups):
            if (g * per + per) // 2 == step:
                hidden_group(g)
                hids.append(exchange(hid_ref, g, hid_sems))

    moe_step = (half + 1) // 2
    for step in range(1, half + 1):
        later = []
        for piece in (0, 1):
            wait_recv(kv_now[piece])
            if step < half:
                later.append(start(kv_copies(step + 1, piece)))
                sent += later[-1]
        kv_now = later
        if step == 1:
            relays += relay(hid_ref, groups - 1, hid_sems, hids[-1])
        if step == moe_step:
            loads[5].wait()
            for copies in hids:
                copies[0].wait_recv()
            wait_recv(relays)

            @pl.loop(0, groups)
            def _(g):
                rows = pl.ds(pl.multiple_of(g * size, size), size)
                total = jnp.zeros((size, moe_ref.shape[1]), f32)
                for t in range(parts):
                    total += jnp.dot(
                        hid[t, rows, :],
                        wdown_ref[t * local : (t + 1) * local, :],
                        preferred_element_type=f32,
                    )
                res[rows, :] = total.astype(bf16)

            ret[me] = res[0:cap, :]
            rets = []
            for slot in range(1, n):
                b = slot_block(slot)
                d = (slot + 1) // 2 if slot % 2 == 1 else n - slot // 2
                rets.append(
                    push(
                        res.at[pl.ds(slot * cap, cap)],
                        ret.at[me],
                        ret_s.at[d],
                        ret_r.at[d],
                        {"ep": b},
                    )
                )
            sent += start(rets)
        attend_step(step)

    @pl.loop(0, width // (2 * head_size))
    def _(h):
        cols = pl.ds(pl.multiple_of(h * 2 * head_size, 2 * head_size), 2 * head_size)
        first = numer[0, :, cols] / denom[0, h][:, :1]
        second = numer[1, :, cols] / denom[1, h][:, :1]
        mix = first - lam_ref[h] * second
        heads[mine, :, cols] = (rms_rows(mix, hgain_ref[...], 1e-05) * 0.8).astype(bf16)

    outs = exchange(head_ref, 0, head_sems)
    passed = relay(head_ref, 0, head_sems, outs)
    for copies in hids:
        sent += copies
    sent += relays + outs + passed

    wait_recv(rets)
    total = jnp.zeros(moe_ref.shape, f32)
    notes = info_ref[...]
    for e in range(n):
        chosen, named = slot_rows(notes, float(e))
        weight = jnp.sum(jnp.where(named, notes[top:, :], 0.0), axis=0, keepdims=True)
        picked = lax.dot_general(
            chosen, ret[e], (((0,), (0,)), ((), ())), preferred_element_type=f32
        )
        total += picked * weight.T
    moe_ref[...] = total.astype(bf16)

    loads[6].wait()
    outs[0].wait_recv()
    wait_recv(passed)
    result = jnp.zeros(attn_ref.shape, f32)
    for t in range(parts):
        result += jnp.dot(
            heads[t], wout_ref[t * width : (t + 1) * width, :], preferred_element_type=f32
        )
    attn_ref[...] = result.astype(bf16)
    for copy in sent:
        copy.wait_send()


def body(
    x_mix,
    mix_gain,
    w_query,
    w_key,
    w_value,
    query_gain,
    key_gain,
    mix_lambda,
    head_gain,
    w_mix_out,
    x_exp,
    exp_gain,
    routes,
    route_weight,
    w_gate,
    w_up,
    w_down,
):
    n, parts = lax.axis_size("ep"), lax.axis_size("tp")
    rows_a = x_mix.shape[0]
    rows_b, model = x_exp.shape
    head_size = query_gain.shape[0]
    width = w_query.shape[1]
    local = w_gate.shape[2]
    out_width = w_down.shape[2]
    head_count = width // (2 * head_size)
    top = routes.shape[1]
    cap = 3 * rows_b * top // (2 * n)
    cap = -(-cap // 16) * 16
    f32, bf16 = jnp.float32, jnp.bfloat16
    wide = min(256, width)
    gains = jnp.tile(jnp.stack([query_gain, key_gain]), (1, wide // head_size))
    info = jnp.concatenate([routes.astype(f32), route_weight], axis=1).T
    vmem = pl.BlockSpec(memory_space=pltpu.VMEM)
    smem = pl.BlockSpec(memory_space=pltpu.SMEM)
    hbm = pl.BlockSpec(memory_space=pl.ANY)
    dma = pltpu.SemaphoreType.DMA
    groups = 4
    return pl.pallas_call(
        functools.partial(kernel, n, parts, top, cap, head_size),
        out_shape=(
            jax.ShapeDtypeStruct((rows_a, w_mix_out.shape[1]), bf16),
            jax.ShapeDtypeStruct((rows_b, out_width), bf16),
        ),
        in_specs=[vmem] * 6 + [smem, vmem] + [hbm] * 7,
        out_specs=(vmem, vmem),
        scratch_shapes=[
            pltpu.VMEM(w_query.shape, bf16),
            pltpu.VMEM(w_key.shape, bf16),
            pltpu.VMEM(w_value.shape, bf16),
            pltpu.VMEM(w_gate.shape[1:], bf16),
            pltpu.VMEM(w_up.shape[1:], bf16),
            pltpu.VMEM(w_down.shape[1:], bf16),
            pltpu.VMEM(w_mix_out.shape, bf16),
            dma((7,)),
            pltpu.VMEM((rows_a, model), bf16),
            pltpu.VMEM((rows_a, width), bf16),
            pltpu.VMEM((rows_a, 2 * width), bf16),
            pltpu.VMEM((rows_b, model), bf16),
            pltpu.VMEM((n, rows_a, 2 * width), bf16),
            pltpu.VMEM((n, rows_b, model), bf16),
            pltpu.VMEM((n, 2 * top, rows_b), f32),
            pltpu.VMEM((n * cap, model), bf16),
            pltpu.VMEM((parts, n * cap, local), bf16),
            pltpu.VMEM((n * cap, out_width), bf16),
            pltpu.VMEM((n, cap, out_width), bf16),
            pltpu.VMEM((2, rows_a, width), f32),
            pltpu.VMEM((2, head_count, rows_a, 128), f32),
            pltpu.VMEM((parts, rows_a, width), bf16),
            dma((2 * n,)),
            dma((2 * n,)),
            dma((n,)),
            dma((n,)),
            dma((2 * n,)),
            dma((2 * n,)),
            dma((2 * n,)),
            dma((2 * n,)),
            dma((groups * parts,)),
            dma((groups * parts,)),
            dma((n,)),
            dma((n,)),
            dma((parts,)),
            dma((parts,)),
        ],
        compiler_params=pltpu.CompilerParams(
            collective_id=0, has_side_effects=True, vmem_limit_bytes=60 * 1024 * 1024
        ),
    )(
        x_mix,
        mix_gain.reshape(1, -1),
        x_exp,
        exp_gain.reshape(1, -1),
        gains,
        info,
        mix_lambda,
        head_gain.reshape(1, -1),
        w_query,
        w_key,
        w_value,
        w_gate,
        w_up,
        w_down,
        w_mix_out,
    )


def solution(mesh):
    return jax.shard_map(
        body,
        mesh=mesh,
        in_specs=(
            P("ep", None),
            P(),
            P(None, "tp"),
            P(None, "tp"),
            P(None, "tp"),
            P(),
            P(),
            P("tp"),
            P(),
            P(None, "tp"),
            P("ep", None),
            P(),
            P("ep", None),
            P("ep", None),
            P("ep", None, "tp"),
            P("ep", None, "tp"),
            P("ep", None, "tp"),
        ),
        out_specs=(P("ep", "tp"), P("ep", "tp")),
        check_vma=False,
    )
```
